1024 devices in a mesh: rep: 4 (over z_hi), fs: 32 (over z_lo, y), tp: 8 (over x, core).
Axes of the slice: x: 4, y: 4, z: 32 (z_hi: 4, z_lo: 8; z = z_hi * 8 + z_lo), core: 2. Of those that a mesh axis runs over, the one named last changes fastest.
Arguments:
- tokens: bfloat16 [65536, 2048], P(('rep', 'fs')), may hold values from -6 to 6
- mix_gain: float32 [2048], replicated, may hold values from 0.1 to 1.9
- w_gate_b: bfloat16 [2048, 1024], P('fs', 'tp'), may hold values from -0.125 to 0.125
- w_gate_c: bfloat16 [2048, 1024], P('fs', 'tp'), may hold values from -0.125 to 0.125
- w_conv_in: bfloat16 [2048, 1024], P('fs', 'tp'), may hold values from -0.125 to 0.125
- conv_taps: float32 [3, 1024], P(None, 'tp'), may hold values from -3 to 3
- w_mix_out: bfloat16 [1024, 2048], P('tp', 'fs'), may hold values from -0.1875 to 0.1875
- ffn_gain: float32 [2048], replicated, may hold values from 0.1 to 1.9
- w_ffn_gate: bfloat16 [2048, 2816], P('fs', 'tp'), may hold values from -0.125 to 0.125
- w_ffn_up: bfloat16 [2048, 2816], P('fs', 'tp'), may hold values from -0.125 to 0.125
- w_ffn_down: bfloat16 [2816, 2048], P('tp', 'fs'), may hold values from -0.109375 to 0.109375
Outputs:
- layer_out: bfloat16 [65536, 2048], P(('rep', 'fs', 'tp'))
The draws below stay inside these ranges and needn't reach their ends.
All inputs are finite; a program needn't handle non-finite values.
Results may differ from the reference program's by a relative error of at most 0.014.
Values may be sent and summed in bfloat16 or wider, within the bound.
No kernel may reach another device: no remote copies, remote signals or barrier semaphores. Data moves between devices by JAX's collectives and lax.ppermute only.
A program may use at most 32 MiB of HBM per device.

```python
import jax
import jax.numpy as jnp
from jax import lax

D = 2048
DC = 1024
FF = 2816
LEN = 128
TOKENS = 65536
N_TP = 8


def shard_levels(own_key, shape, pieces, smallest, top_value):
    loudness = 1.0
    for dim, parts in pieces:
        draws = jax.random.uniform(jax.random.fold_in(jax.random.fold_in(own_key, 6), dim), (parts,), jnp.float32, smallest / len(pieces), top_value / len(pieces))
        loudness = loudness * jnp.repeat(jnp.exp(draws), shape[dim] // parts).reshape((-1,) + (1,) * (len(shape) - 1 - dim))
    return loudness


def gaussian(rng, shape, scale, limit, cuts=(), held_as=jnp.bfloat16):
    loudness = shard_levels(rng, shape, cuts, -0.22, 0.18) if cuts else 1.0
    values = jax.random.normal(rng, shape, jnp.float32) * scale * loudness
    return jnp.minimum(jnp.maximum(values, -limit), limit).astype(held_as)


def setup_inputs(seed: int = 0) -> dict:
    keys = jax.random.split(jax.random.key(seed), 12)
    tokens = gaussian(keys[0], (TOKENS, D), 1.0, 6.0, ((0, 128),))
    mix_gain = jnp.clip(1.0 + 0.18 * jax.random.normal(keys[1], (D,), jnp.float32), 0.1, 1.9)
    w_gate_b = gaussian(keys[2], (D, DC), D ** -0.5, 0.125, ((0, 32), (1, 8)))
    w_gate_c = gaussian(keys[3], (D, DC), D ** -0.5, 0.125, ((0, 32), (1, 8)))
    w_conv_in = gaussian(keys[4], (D, DC), D ** -0.5, 0.125, ((0, 32), (1, 8)))
    conv_taps = gaussian(keys[5], (3, DC), 0.6, 3.0, ((1, 8),), jnp.float32)
    w_mix_out = gaussian(keys[6], (DC, D), DC ** -0.5, 0.1875, ((0, 8), (1, 32)))
    ffn_gain = jnp.clip(1.0 + 0.18 * jax.random.normal(keys[7], (D,), jnp.float32), 0.1, 1.9)
    w_ffn_gate = gaussian(keys[8], (D, FF), D ** -0.5, 0.125, ((0, 32), (1, 8)))
    w_ffn_up = gaussian(keys[9], (D, FF), D ** -0.5, 0.125, ((0, 32), (1, 8)))
    w_ffn_down = gaussian(keys[10], (FF, D), FF ** -0.5, 0.109375, ((0, 8), (1, 32)))
    return {"tokens": tokens, "mix_gain": mix_gain, "w_gate_b": w_gate_b, "w_gate_c": w_gate_c, "w_conv_in": w_conv_in, "conv_taps": conv_taps, "w_mix_out": w_mix_out, "ffn_gain": ffn_gain, "w_ffn_gate": w_ffn_gate, "w_ffn_up": w_ffn_up, "w_ffn_down": w_ffn_down}


EPSILON = 1e-06

def rms_scale(values, gain):
    return values * lax.rsqrt(lax.optimization_barrier(jnp.mean(values * values, axis=-1, keepdims=True)) + EPSILON) * gain

def causal_mix(product_in, conv_taps):
    shaped = product_in.reshape(product_in.shape[0] // LEN, LEN, product_in.shape[1])
    padded = jnp.pad(shaped, ((0, 0), (2, 0), (0, 0)))
    convolved = conv_taps[0] * padded[:, :-2] + conv_taps[1] * padded[:, 1:-1] + conv_taps[2] * padded[:, 2:]
    return convolved.reshape(product_in.shape)

def block_sum(acts, weight, blocks):
    block_width = acts.shape[1] // blocks

    def step(running, block_index):
        first = (block_index * block_width).astype(jnp.int32)
        partial_value = jnp.dot(lax.dynamic_slice_in_dim(acts, first, block_width, 1), lax.dynamic_slice_in_dim(weight, first, block_width, 0), preferred_element_type=jnp.float32)
        rounded = lax.optimization_barrier(partial_value.astype(jnp.bfloat16)).astype(jnp.float32)
        return (running + rounded, None)
    start_acc = jnp.zeros((acts.shape[0], weight.shape[1]), jnp.float32)
    running, _ = lax.scan(step, start_acc, jnp.arange(blocks, dtype=jnp.int32))
    return running

def reference(tokens, mix_gain, w_gate_b, w_gate_c, w_conv_in, conv_taps, w_mix_out, ffn_gain, w_ffn_gate, w_ffn_up, w_ffn_down):
    inputs = tokens.astype(jnp.float32)
    normed = rms_scale(inputs, mix_gain).astype(jnp.bfloat16)
    gate_b = jnp.dot(normed, w_gate_b, preferred_element_type=jnp.float32)
    gate_c = jnp.dot(normed, w_gate_c, preferred_element_type=jnp.float32)
    conv_in = jnp.dot(normed, w_conv_in, preferred_element_type=jnp.float32)
    convolved = causal_mix(gate_c * conv_in, conv_taps)
    gated = (gate_b * convolved).astype(jnp.bfloat16)
    stream = inputs + block_sum(gated, w_mix_out, N_TP)
    normed_two = rms_scale(stream, ffn_gain).astype(jnp.bfloat16)
    gate_part = jnp.dot(normed_two, w_ffn_gate, preferred_element_type=jnp.float32)
    up_part = jnp.dot(normed_two, w_ffn_up, preferred_element_type=jnp.float32)
    hidden = (jax.nn.silu(gate_part) * up_part).astype(jnp.bfloat16)
    return (stream + block_sum(hidden, w_ffn_down, N_TP)).astype(jnp.bfloat16)
```

```python
import jax
import jax.numpy as jnp
from jax import lax
from jax.experimental import pallas as pl
from jax.experimental.pallas import tpu as pltpu
from jax.sharding import Mesh, PartitionSpec as P

LEN = 128
EPSILON = 1e-06
Z_LO = 8
Z = ("rep", "zl")
SWAP = [(0, 1), (1, 0)]

VMEM = pl.BlockSpec(memory_space=pltpu.VMEM)
SMEM = pl.BlockSpec(memory_space=pltpu.SMEM)


def shift(value, axis, size, distance):
    return lax.ppermute(value, axis, [((k + distance) % size, k) for k in range(size)])


def exchange(blocks, axis):
    return lax.all_to_all(blocks, axis, 0, 0, tiled=True)


def copies(array, count):
    return jnp.broadcast_to(array[None], (count, *array.shape))


def rms_scale(values, gain):
    return values * lax.rsqrt(jnp.mean(values * values, axis=-1, keepdims=True) + EPSILON) * gain


def dot_t(acts, weight_t):
    return lax.dot_general(acts, weight_t, (((1,), (1,)), ((), ())), preferred_element_type=jnp.float32)


def dot(acts, weight):
    return jnp.dot(acts, weight, preferred_element_type=jnp.float32)


def call(kernel, outs, pos, args, mib, scratch=()):
    args = [pltpu.with_memory_space_constraint(a, pltpu.VMEM) for a in args]
    specs = [VMEM] * len(args)
    if pos is not None:
        args, specs = [pos, *args], [SMEM, *specs]
    return pl.pallas_call(
        kernel,
        out_shape=outs,
        in_specs=specs,
        out_specs=(VMEM,) * len(outs),
        scratch_shapes=scratch,
        compiler_params=pltpu.CompilerParams(vmem_limit_bytes=mib * 1024 * 1024),
    )(*args)


def mixer_kernel(places, n_y, pos, normed, taps, gathered, mine, other, weights, gated):
    zl, core = pos[0], pos[1]
    rows = gathered.shape[2]
    width = taps.shape[1]
    for k, d in enumerate(places):
        z = lax.rem(zl + (d + Z_LO), Z_LO)
        for y in range(n_y):
            first = pl.multiple_of((z * n_y + y) * rows, rows)
            weights[pl.ds(first, rows), :] = gathered[y, k]
    products = dot(normed[...], weights[:, : 3 * width])
    p = products[:, width : 2 * width] * products[:, 2 * width : 3 * width]
    place = lax.broadcasted_iota(jnp.int32, p.shape, 0) % LEN
    before = jnp.where(place >= 1, pltpu.roll(p, 1, 0), 0.0)
    before_two = jnp.where(place >= 2, pltpu.roll(p, 2, 0), 0.0)
    convolved = taps[0:1, :] * before_two + taps[1:2, :] * before + taps[2:3, :] * p
    gated[...] = (products[:, :width] * convolved).astype(jnp.bfloat16)
    out_t = weights[:, 3 * width :]
    n_x = mine.shape[0]
    step = mine.shape[1]
    for half, out in ((core, mine), (1 - core, other)):
        for x in range(n_x):
            first = pl.multiple_of(x * 2 * step + half * step, step)
            out[x] = dot_t(gated[pl.ds(first, step), :], out_t).astype(jnp.bfloat16)


def tick_kernel(pos, out):
    for k in range(pos.shape[0]):
        out[k] = pos[k]


def tick(pos):
    return pl.pallas_call(
        tick_kernel,
        out_shape=jax.ShapeDtypeStruct(pos.shape, pos.dtype),
        in_specs=[SMEM],
        out_specs=SMEM,
        compiler_params=pltpu.CompilerParams(vmem_limit_bytes=1024 * 1024),
    )(pos)


def join_kernel(blocks, own, gain, stream, sent):
    total = own[...].astype(jnp.float32)
    for k in range(blocks.shape[0]):
        total += blocks[k].astype(jnp.float32)
    stream[...] = total
    normed = rms_scale(total, gain[...]).astype(jnp.bfloat16)
    for k in range(sent.shape[0]):
        sent[k] = normed


def last_kernel(blocks, stream, out):
    total = stream[...]
    for k in range(blocks.shape[0]):
        total += blocks[k].astype(jnp.float32)
    out[...] = total.astype(jnp.bfloat16)


def ffn_kernel(places, n_ff, down_at, pos, acts, *refs):
    chunks, out = refs[: len(places)], refs[len(places)]
    depth = acts.shape[1] // Z_LO
    both = None
    firsts = []
    for (d, row), chunk in zip(places, chunks):
        z = lax.rem(pos[0] + (d + Z_LO), Z_LO)
        first = pl.multiple_of(z * depth + row, chunk.shape[0])
        firsts.append(first)
        part = dot(acts[:, pl.ds(first, chunk.shape[0])], chunk[:, : 2 * n_ff])
        both = part if both is None else both + part
    hidden = (jax.nn.silu(both[:, :n_ff]) * both[:, n_ff:]).astype(jnp.bfloat16)
    for first, chunk in zip(firsts, chunks):
        part = dot_t(hidden, chunk[:, down_at : down_at + n_ff])
        out[:, pl.ds(first, chunk.shape[0])] = part.astype(jnp.bfloat16)


def local(
    tokens,
    mix_gain,
    w_gate_b,
    w_gate_c,
    w_conv_in,
    conv_taps,
    w_mix_out,
    ffn_gain,
    w_ffn_gate,
    w_ffn_up,
    w_ffn_down,
):
    nx, ny = lax.axis_size("x"), lax.axis_size("y")
    nz = lax.axis_size("rep") * lax.axis_size("zl")
    zl, core = lax.axis_index("zl"), lax.axis_index("core")
    pos = jnp.stack([zl, core]).astype(jnp.int32)
    count, feats = tokens.shape
    half_rows = count // 2
    own_rows = half_rows // nx

    mixer = jnp.concatenate([w_gate_b, w_gate_c, w_conv_in, w_mix_out.T], axis=1)
    places = [0, 4, 3, -3, 2, -2, 1, -1]
    held = [mixer] + [shift(mixer, Z, nz, d) for k, d in enumerate(places) if k]

    n_ff = w_ffn_gate.shape[1]
    down_at = -(-2 * n_ff // 128) * 128
    width = -(-(down_at + n_ff) // 128) * 128
    ffn = jnp.concatenate([w_ffn_gate, w_ffn_up], axis=1)
    ffn = jnp.concatenate(
        [jnp.pad(ffn, ((0, 0), (0, down_at - 2 * n_ff))), jnp.pad(w_ffn_down.T, ((0, 0), (0, width - down_at - n_ff)))],
        axis=1,
    )
    ffn_y = exchange(copies(ffn, ny), "y").reshape(-1, width)
    chunks, ffn_places = [ffn_y], [(0, 0)]
    up = down = ffn_y
    for k in (1, 2, 3):
        up, down = shift(up, Z, nz, 1), shift(down, Z, nz, -1)
        chunks += [up, down]
        ffn_places += [(k, 0), (-k, 0)]
    cut = ffn_y.shape[0] // 2
    chunks += [shift(up[:cut], Z, nz, 1), shift(down[cut:], Z, nz, -1)]
    ffn_places += [(4, 0), (4, cut)]

    normed = rms_scale(tokens.astype(jnp.float32), mix_gain).astype(jnp.bfloat16)
    own = lax.dynamic_slice_in_dim(tokens, (lax.axis_index("x") * 2 + core) * own_rows, own_rows, 0)
    held, normed, own = lax.optimization_barrier((jnp.stack(held), normed, own))
    gathered = exchange(copies(held, ny), "y").reshape(ny, Z_LO, *mixer.shape)

    bf, f32 = jnp.bfloat16, jnp.float32
    halves = (nx, own_rows, feats)

    def mixer_body(*refs):
        mixer_kernel(places, ny, *refs)

    pos = tick(tick(pos))
    scratch = [pltpu.VMEM((feats, mixer.shape[1]), bf), pltpu.VMEM((count, w_gate_b.shape[1]), bf)]
    mine, other = call(mixer_body, (pltpu.VMEM(halves, bf),) * 2, pos, (normed, conv_taps, gathered), 16, scratch)

    def over_tp(mine, other):
        got = lax.ppermute(other, "core", SWAP)
        pair = (mine.astype(f32) + got.astype(f32)).astype(bf)
        return exchange(pair, "x")

    pos = tick(pos)
    blocks = over_tp(mine, other)
    stream, sent = call(
        join_kernel,
        (pltpu.VMEM((own_rows, feats), f32), jax.ShapeDtypeStruct(halves, bf)),
        None,
        (blocks, own, ffn_gain.reshape(1, -1)),
        8,
    )
    pos = tick(pos)
    acts = exchange(sent, "x").reshape(half_rows, feats)
    acts_other = lax.ppermute(acts, "core", SWAP)

    def ffn_body(*refs):
        ffn_kernel(ffn_places, n_ff, down_at, *refs)

    def feed_forward(values):
        (out,) = call(ffn_body, (pltpu.VMEM((half_rows, feats), bf),), pos, (values, *chunks), 12)
        return out.reshape(nx, own_rows, feats)

    ffn_mine = feed_forward(acts)
    acts_other, ffn_mine = lax.optimization_barrier((acts_other, ffn_mine))
    blocks = over_tp(ffn_mine, feed_forward(acts_other))
    return call(last_kernel, (jax.ShapeDtypeStruct((own_rows, feats), bf),), None, (blocks, stream), 8)[0]


def solution(mesh):
    fine = Mesh(
        mesh.devices.reshape(mesh.shape["rep"], Z_LO, mesh.shape["fs"] // Z_LO, mesh.shape["tp"] // 2, 2),
        ("rep", "zl", "y", "x", "core"),
    )
    fs, tp = ("zl", "y"), ("x", "core")
    in_specs = (
        P(("rep", *fs), None),
        P(),
        P(fs, tp),
        P(fs, tp),
        P(fs, tp),
        P(None, tp),
        P(tp, fs),
        P(),
        P(fs, tp),
        P(fs, tp),
        P(tp, fs),
    )
    out_specs = P(("rep", *fs, *tp), None)
    return jax.shard_map(local, mesh=fine, in_specs=in_specs, out_specs=out_specs, check_vma=False)
```

```python
import jax
import jax.numpy as jnp
from jax import lax
from jax.experimental import pallas as pl
from jax.experimental.pallas import tpu as pltpu
from jax.sharding import Mesh, PartitionSpec as P

LEN = 128
EPSILON = 1e-06
Z_LO = 8
Z = ("rep", "zl")
SWAP = [(0, 1), (1, 0)]

VMEM = pl.BlockSpec(memory_space=pltpu.VMEM)
SMEM = pl.BlockSpec(memory_space=pltpu.SMEM)


def shift(value, axis, size, distance):
    return lax.ppermute(value, axis, [((k + distance) % size, k) for k in range(size)])


def exchange(blocks, axis):
    return lax.all_to_all(blocks, axis, 0, 0, tiled=True)


def rms_scale(values, gain):
    return values * lax.rsqrt(jnp.mean(values * values, axis=-1, keepdims=True) + EPSILON) * gain


def dot_t(acts, weight_t):
    return lax.dot_general(acts, weight_t, (((1,), (1,)), ((), ())), preferred_element_type=jnp.float32)


def dot(acts, weight):
    return jnp.dot(acts, weight, preferred_element_type=jnp.float32)


def call(kernel, outs, pos, args, mib, scratch=()):
    args = [pltpu.with_memory_space_constraint(a, pltpu.VMEM) for a in args]
    specs = [VMEM] * len(args)
    if pos is not None:
        args, specs = [pos, *args], [SMEM, *specs]
    return pl.pallas_call(
        kernel,
        out_shape=outs,
        in_specs=specs,
        out_specs=(VMEM,) * len(outs),
        scratch_shapes=scratch,
        compiler_params=pltpu.CompilerParams(vmem_limit_bytes=mib * 1024 * 1024),
    )(*args)


def mixer_kernel(places, n_y, pos, normed, taps, gathered, mine, other, weights, gated):
    zl, core = pos[0], pos[1]
    rows = gathered.shape[2]
    width = taps.shape[1]
    for k, d in enumerate(places):
        z = lax.rem(zl + (d + Z_LO), Z_LO)
        for y in range(n_y):
            first = pl.multiple_of((z * n_y + y) * rows, rows)
            weights[pl.ds(first, rows), :] = gathered[y, k]
    products = dot(normed[...], weights[:, : 3 * width])
    p = products[:, width : 2 * width] * products[:, 2 * width : 3 * width]
    place = lax.broadcasted_iota(jnp.int32, p.shape, 0) % LEN
    before = jnp.where(place >= 1, pltpu.roll(p, 1, 0), 0.0)
    before_two = jnp.where(place >= 2, pltpu.roll(p, 2, 0), 0.0)
    convolved = taps[0:1, :] * before_two + taps[1:2, :] * before + taps[2:3, :] * p
    gated[...] = (products[:, :width] * convolved).astype(jnp.bfloat16)
    out_t = weights[:, 3 * width :]
    n_x = mine.shape[0]
    step = mine.shape[1]
    for half, out in ((core, mine), (1 - core, other)):
        for x in range(n_x):
            first = pl.multiple_of(x * 2 * step + half * step, step)
            out[x] = dot_t(gated[pl.ds(first, step), :], out_t).astype(jnp.bfloat16)


def tick_kernel(pos, out):
    for k in range(pos.shape[0]):
        out[k] = pos[k]


def tick(pos):
    return pl.pallas_call(
        tick_kernel,
        out_shape=jax.ShapeDtypeStruct(pos.shape, pos.dtype),
        in_specs=[SMEM],
        out_specs=SMEM,
        compiler_params=pltpu.CompilerParams(vmem_limit_bytes=1024 * 1024),
    )(pos)


def norm_kernel(tokens, gain, normed):
    normed[...] = rms_scale(tokens[...].astype(jnp.float32), gain[...]).astype(jnp.bfloat16)


def stack_kernel(*refs):
    for k, block in enumerate(refs[:-1]):
        refs[-1][0, k] = block[...]


def bundle_kernel(*refs):
    out = refs[-1]
    out[...] = jnp.zeros(out.shape, out.dtype)
    step = out.shape[2] // (len(refs) - 1)
    for k, array in enumerate(refs[:-1]):
        out[0, :, k * step : k * step + array.shape[1]] = array[...]


def for_exchange(kernel, args, count, shape, dtype):
    args = [pltpu.with_memory_space_constraint(a, pltpu.VMEM) for a in args]
    zeros = (0,) * len(shape)
    return pl.pallas_call(
        kernel,
        grid=(count,),
        out_shape=pltpu.HBM((count, *shape), dtype),
        in_specs=[VMEM] * len(args),
        out_specs=pl.BlockSpec((1, *shape), lambda k: (k, *zeros)),
        compiler_params=pltpu.CompilerParams(vmem_limit_bytes=8 * 1024 * 1024),
    )(*args)


def join_kernel(blocks, own, gain, stream, sent):
    total = own[...].astype(jnp.float32)
    for k in range(blocks.shape[0]):
        total += blocks[k].astype(jnp.float32)
    stream[...] = total
    normed = rms_scale(total, gain[...]).astype(jnp.bfloat16)
    for k in range(sent.shape[0]):
        sent[k] = normed


def last_kernel(blocks, stream, out):
    total = stream[...]
    for k in range(blocks.shape[0]):
        total += blocks[k].astype(jnp.float32)
    out[...] = total.astype(jnp.bfloat16)


def ffn_kernel(places, n_ff, pos, acts, *refs):
    chunks, out = refs[: len(places)], refs[len(places)]
    depth = acts.shape[1] // Z_LO
    step = chunks[0].shape[1] // 3
    both = None
    firsts = []
    for (d, row), chunk in zip(places, chunks):
        z = lax.rem(pos[0] + (d + Z_LO), Z_LO)
        first = pl.multiple_of(z * depth + row, chunk.shape[0])
        firsts.append(first)
        part = dot(acts[:, pl.ds(first, chunk.shape[0])], chunk[:, : 2 * step])
        both = part if both is None else both + part
    hidden = (jax.nn.silu(both[:, :n_ff]) * both[:, step : step + n_ff]).astype(jnp.bfloat16)
    for first, chunk in zip(firsts, chunks):
        part = dot_t(hidden, chunk[:, 2 * step : 2 * step + n_ff])
        out[:, pl.ds(first, chunk.shape[0])] = part.astype(jnp.bfloat16)


def local(
    tokens,
    mix_gain,
    w_gate_b,
    w_gate_c,
    w_conv_in,
    conv_taps,
    w_mix_out,
    ffn_gain,
    w_ffn_gate,
    w_ffn_up,
    w_ffn_down,
):
    nx, ny = lax.axis_size("x"), lax.axis_size("y")
    nz = lax.axis_size("rep") * lax.axis_size("zl")
    zl, core = lax.axis_index("zl"), lax.axis_index("core")
    pos = jnp.stack([zl, core]).astype(jnp.int32)
    count, feats = tokens.shape
    half_rows = count // 2
    own_rows = half_rows // nx

    mixer = jnp.concatenate([w_gate_b, w_gate_c, w_conv_in, w_mix_out.T], axis=1)
    places = [0, 4, 3, -3, 2, -2, 1, -1]
    held = [mixer] + [shift(mixer, Z, nz, d) for k, d in enumerate(places) if k]

    n_ff = w_ffn_gate.shape[1]
    width = 3 * (-(-n_ff // 128) * 128)
    sent_ffn = for_exchange(
        bundle_kernel, (w_ffn_gate, w_ffn_up, w_ffn_down.T), ny, (w_ffn_gate.shape[0], width), w_ffn_gate.dtype
    )
    ffn_y = exchange(sent_ffn, "y").reshape(-1, width)
    chunks, ffn_places = [ffn_y], [(0, 0)]
    up = down = ffn_y
    for k in (1, 2, 3):
        up, down = shift(up, Z, nz, 1), shift(down, Z, nz, -1)
        chunks += [up, down]
        ffn_places += [(k, 0), (-k, 0)]
    cut = ffn_y.shape[0] // 2
    chunks += [shift(up[:cut], Z, nz, 1), shift(down[cut:], Z, nz, -1)]
    ffn_places += [(4, 0), (4, cut)]

    own = lax.dynamic_slice_in_dim(tokens, (lax.axis_index("x") * 2 + core) * own_rows, own_rows, 0)
    sent_mixer = for_exchange(stack_kernel, held, ny, (Z_LO, *mixer.shape), mixer.dtype)
    gathered = exchange(sent_mixer.reshape(-1, *mixer.shape), "y").reshape(ny, Z_LO, *mixer.shape)

    bf, f32 = jnp.bfloat16, jnp.float32
    halves = (nx, own_rows, feats)

    def mixer_body(*refs):
        mixer_kernel(places, ny, *refs)

    (normed,) = call(norm_kernel, (jax.ShapeDtypeStruct(tokens.shape, bf),), None, (tokens, mix_gain.reshape(1, -1)), 12)
    pos = tick(pos)
    scratch = [pltpu.VMEM((feats, mixer.shape[1]), bf), pltpu.VMEM((count, w_gate_b.shape[1]), bf)]
    mine, other = call(mixer_body, (pltpu.VMEM(halves, bf),) * 2, pos, (normed, conv_taps, gathered), 16, scratch)

    def over_tp(mine, other):
        got = lax.ppermute(other, "core", SWAP)
        pair = (mine.astype(f32) + got.astype(f32)).astype(bf)
        return exchange(pair, "x")

    pos = tick(pos)
    blocks = over_tp(mine, other)
    stream, sent = call(
        join_kernel,
        (jax.ShapeDtypeStruct((own_rows, feats), f32), pltpu.HBM(halves, bf)),
        None,
        (blocks, own, ffn_gain.reshape(1, -1)),
        8,
    )
    pos = tick(pos)
    acts = exchange(sent, "x").reshape(half_rows, feats)
    acts_other = lax.ppermute(acts, "core", SWAP)

    def ffn_body(*refs):
        ffn_kernel(ffn_places, n_ff, *refs)

    def feed_forward(values):
        (out,) = call(ffn_body, (pltpu.VMEM((half_rows, feats), bf),), pos, (values, *chunks), 12)
        return out.reshape(nx, own_rows, feats)

    ffn_mine = feed_forward(acts)
    acts_other, ffn_mine = lax.optimization_barrier((acts_other, ffn_mine))
    blocks = over_tp(ffn_mine, feed_forward(acts_other))
    return call(last_kernel, (jax.ShapeDtypeStruct((own_rows, feats), bf),), None, (blocks, stream), 8)[0]


def solution(mesh):
    fine = Mesh(
        mesh.devices.reshape(mesh.shape["rep"], Z_LO, mesh.shape["fs"] // Z_LO, mesh.shape["tp"] // 2, 2),
        ("rep", "zl", "y", "x", "core"),
    )
    fs, tp = ("zl", "y"), ("x", "core")
    in_specs = (
        P(("rep", *fs), None),
        P(),
        P(fs, tp),
        P(fs, tp),
        P(fs, tp),
        P(None, tp),
        P(tp, fs),
        P(),
        P(fs, tp),
        P(fs, tp),
        P(tp, fs),
    )
    out_specs = P(("rep", *fs, *tp), None)
    return jax.shard_map(local, mesh=fine, in_specs=in_specs, out_specs=out_specs, check_vma=False)
```

```python
import jax
import jax.numpy as jnp
from jax import lax
from jax.experimental import pallas as pl
from jax.experimental.pallas import tpu as pltpu
from jax.sharding import Mesh, PartitionSpec as P

LEN = 128
EPSILON = 1e-06
Z_LO = 8
Z = ("rep", "zl")
SWAP = [(0, 1), (1, 0)]

VMEM = pl.BlockSpec(memory_space=pltpu.VMEM)
SMEM = pl.BlockSpec(memory_space=pltpu.SMEM)


def shift(value, axis, size, distance):
    return lax.ppermute(value, axis, [((k + distance) % size, k) for k in range(size)])


def exchange(blocks, axis):
    return lax.all_to_all(blocks, axis, 0, 0, tiled=True)


def rms_scale(values, gain):
    return values * lax.rsqrt(jnp.mean(values * values, axis=-1, keepdims=True) + EPSILON) * gain


def dot_t(acts, weight_t):
    return lax.dot_general(acts, weight_t, (((1,), (1,)), ((), ())), preferred_element_type=jnp.float32)


def dot(acts, weight):
    return jnp.dot(acts, weight, preferred_element_type=jnp.float32)


def call(kernel, outs, pos, args, mib, scratch=()):
    args = [pltpu.with_memory_space_constraint(a, pltpu.VMEM) for a in args]
    specs = [VMEM] * len(args)
    if pos is not None:
        args, specs = [pos, *args], [SMEM, *specs]
    return pl.pallas_call(
        kernel,
        out_shape=outs,
        in_specs=specs,
        out_specs=(VMEM,) * len(outs),
        scratch_shapes=scratch,
        compiler_params=pltpu.CompilerParams(vmem_limit_bytes=mib * 1024 * 1024),
    )(*args)


def mixer_kernel(pos, normed, taps, gathered, mine, other, weights, gated):
    core = pos[1]
    n_y, n_z, rows, _ = gathered.shape
    width = taps.shape[1]
    for z in range(n_z):
        for y in range(n_y):
            first = (z * n_y + y) * rows
            weights[first : first + rows, :] = gathered[y, z]
    products = dot(normed[...], weights[:, : 3 * width])
    p = products[:, width : 2 * width] * products[:, 2 * width : 3 * width]
    place = lax.broadcasted_iota(jnp.int32, p.shape, 0) % LEN
    before = jnp.where(place >= 1, pltpu.roll(p, 1, 0), 0.0)
    before_two = jnp.where(place >= 2, pltpu.roll(p, 2, 0), 0.0)
    convolved = taps[0:1, :] * before_two + taps[1:2, :] * before + taps[2:3, :] * p
    gated[...] = (products[:, :width] * convolved).astype(jnp.bfloat16)
    out_t = weights[:, 3 * width :]
    n_x = mine.shape[0]
    step = mine.shape[1]
    for half, out in ((core, mine), (1 - core, other)):
        for x in range(n_x):
            first = pl.multiple_of(x * 2 * step + half * step, step)
            out[x] = dot_t(gated[pl.ds(first, step), :], out_t).astype(jnp.bfloat16)


def tick_kernel(pos, out):
    for k in range(pos.shape[0]):
        out[k] = pos[k]


def tick(pos):
    return pl.pallas_call(
        tick_kernel,
        out_shape=jax.ShapeDtypeStruct(pos.shape, pos.dtype),
        in_specs=[SMEM],
        out_specs=SMEM,
        compiler_params=pltpu.CompilerParams(vmem_limit_bytes=1024 * 1024),
    )(pos)


def ordered_kernel(places, pos, *refs):
    out = refs[-1]
    for d, block in zip(places, refs[:-1]):
        y = lax.rem(pos[2] + (d + len(places)), len(places))
        out[pl.ds(pl.multiple_of(y * block.shape[0], block.shape[0]), block.shape[0]), :] = block[...]


def copy_kernel(block, out):
    out[0] = block[...]


def bundle_kernel(*refs):
    out = refs[-1]
    out[...] = jnp.zeros(out.shape, out.dtype)
    step = out.shape[2] // (len(refs) - 1)
    for k, array in enumerate(refs[:-1]):
        out[0, :, k * step : k * step + array.shape[1]] = array[...]


def for_exchange(kernel, args, count, shape, dtype, space=pltpu.HBM, source=pltpu.HBM):
    args = [pltpu.with_memory_space_constraint(a, source) for a in args]
    zeros = (0,) * len(shape)
    return pl.pallas_call(
        kernel,
        grid=(count,),
        out_shape=space((count, *shape), dtype),
        in_specs=[VMEM] * len(args),
        out_specs=pl.BlockSpec((1, *shape), lambda k: (k, *zeros)),
        compiler_params=pltpu.CompilerParams(vmem_limit_bytes=8 * 1024 * 1024),
    )(*args)


def join_kernel(blocks, own, gain, stream, sent):
    total = own[...].astype(jnp.float32)
    for k in range(blocks.shape[0]):
        total += blocks[k].astype(jnp.float32)
    stream[...] = total
    normed = rms_scale(total, gain[...]).astype(jnp.bfloat16)
    for k in range(sent.shape[0]):
        sent[k] = normed


def last_kernel(blocks, stream, out):
    total = stream[...]
    for k in range(blocks.shape[0]):
        total += blocks[k].astype(jnp.float32)
    out[...] = total.astype(jnp.bfloat16)


def ffn_kernel(places, n_ff, pos, acts, *refs):
    chunks, out = refs[: len(places)], refs[len(places)]
    depth = acts.shape[1] // Z_LO
    step = chunks[0].shape[1] // 3
    both = None
    firsts = []
    for (d, row), chunk in zip(places, chunks):
        z = lax.rem(pos[0] + (d + Z_LO), Z_LO)
        first = pl.multiple_of(z * depth + row, chunk.shape[0])
        firsts.append(first)
        part = dot(acts[:, pl.ds(first, chunk.shape[0])], chunk[:, : 2 * step])
        both = part if both is None else both + part
    hidden = (jax.nn.silu(both[:, :n_ff]) * both[:, step : step + n_ff]).astype(jnp.bfloat16)
    for first, chunk in zip(firsts, chunks):
        part = dot_t(hidden, chunk[:, 2 * step : 2 * step + n_ff])
        out[:, pl.ds(first, chunk.shape[0])] = part.astype(jnp.bfloat16)


def local(
    tokens,
    mix_gain,
    w_gate_b,
    w_gate_c,
    w_conv_in,
    conv_taps,
    w_mix_out,
    ffn_gain,
    w_ffn_gate,
    w_ffn_up,
    w_ffn_down,
):
    nx, ny = lax.axis_size("x"), lax.axis_size("y")
    nz = lax.axis_size("rep") * lax.axis_size("zl")
    zl, core = lax.axis_index("zl"), lax.axis_index("core")
    pos = jnp.stack([zl, core, lax.axis_index("y")]).astype(jnp.int32)
    count, feats = tokens.shape
    half_rows = count // 2
    own_rows = half_rows // nx

    parts = (w_gate_b, w_gate_c, w_conv_in, w_mix_out.T)
    mixer_shape = (w_gate_b.shape[0], sum(part.shape[1] for part in parts))
    sent = for_exchange(bundle_kernel, parts, Z_LO, mixer_shape, w_gate_b.dtype)
    along_z = exchange(sent, "zl")
    sent = for_exchange(copy_kernel, (along_z,), ny, along_z.shape, along_z.dtype, source=pltpu.VMEM)
    normed = rms_scale(tokens.astype(jnp.float32), mix_gain).astype(jnp.bfloat16)
    own = lax.dynamic_slice_in_dim(tokens, (lax.axis_index("x") * 2 + core) * own_rows, own_rows, 0)
    gathered = exchange(sent.reshape(-1, *mixer_shape), "y").reshape(ny, Z_LO, *mixer_shape)

    n_ff = w_ffn_gate.shape[1]
    width = 3 * (-(-n_ff // 128) * 128)
    ffn_shape = (w_ffn_gate.shape[0], width)
    parts = (w_ffn_gate, w_ffn_up, w_ffn_down.T)
    ffn = for_exchange(bundle_kernel, parts, 1, ffn_shape, w_ffn_gate.dtype, jax.ShapeDtypeStruct)[0]
    y_places = [0, 2, 1, -1]
    blocks = [shift(ffn, "y", ny, d) if d else ffn for d in y_places]

    def ordered_body(*refs):
        ordered_kernel(y_places, *refs)

    (ffn_y,) = call(ordered_body, (jax.ShapeDtypeStruct((ny * ffn_shape[0], width), ffn.dtype),), pos, blocks, 4)
    chunks, ffn_places = [ffn_y], [(0, 0)]
    up = down = ffn_y
    for k in (1, 2, 3):
        up, down = shift(up, Z, nz, 1), shift(down, Z, nz, -1)
        chunks += [up, down]
        ffn_places += [(k, 0), (-k, 0)]
    cut = ffn_y.shape[0] // 2
    chunks += [shift(up[:cut], Z, nz, 1), shift(down[cut:], Z, nz, -1)]
    ffn_places += [(4, 0), (4, cut)]

    bf, f32 = jnp.bfloat16, jnp.float32
    halves = (nx, own_rows, feats)

    pos = tick(pos)
    scratch = [pltpu.VMEM((feats, mixer_shape[1]), bf), pltpu.VMEM((count, w_gate_b.shape[1]), bf)]
    mine, other = call(mixer_kernel, (pltpu.VMEM(halves, bf),) * 2, pos, (normed, conv_taps, gathered), 16, scratch)

    def over_tp(mine, other):
        got = lax.ppermute(other, "core", SWAP)
        pair = (mine.astype(f32) + got.astype(f32)).astype(bf)
        return exchange(pair, "x")

    pos = tick(pos)
    blocks = over_tp(mine, other)
    stream, sent = call(
        join_kernel,
        (jax.ShapeDtypeStruct((own_rows, feats), f32), pltpu.HBM(halves, bf)),
        None,
        (blocks, own, ffn_gain.reshape(1, -1)),
        8,
    )
    pos = tick(pos)
    acts = exchange(sent, "x").reshape(half_rows, feats)
    acts_other = lax.ppermute(acts, "core", SWAP)

    def ffn_body(*refs):
        ffn_kernel(ffn_places, n_ff, *refs)

    def feed_forward(values):
        (out,) = call(ffn_body, (pltpu.VMEM((half_rows, feats), bf),), pos, (values, *chunks), 12)
        return out.reshape(nx, own_rows, feats)

    ffn_mine = feed_forward(acts)
    acts_other, ffn_mine = lax.optimization_barrier((acts_other, ffn_mine))
    blocks = over_tp(ffn_mine, feed_forward(acts_other))
    return call(last_kernel, (jax.ShapeDtypeStruct((own_rows, feats), bf),), None, (blocks, stream), 8)[0]


def solution(mesh):
    fine = Mesh(
        mesh.devices.reshape(mesh.shape["rep"], Z_LO, mesh.shape["fs"] // Z_LO, mesh.shape["tp"] // 2, 2),
        ("rep", "zl", "y", "x", "core"),
    )
    fs, tp = ("zl", "y"), ("x", "core")
    in_specs = (
        P(("rep", *fs), None),
        P(),
        P(fs, tp),
        P(fs, tp),
        P(fs, tp),
        P(None, tp),
        P(tp, fs),
        P(),
        P(fs, tp),
        P(fs, tp),
        P(tp, fs),
    )
    out_specs = P(("rep", *fs, *tp), None)
    return jax.shard_map(local, mesh=fine, in_specs=in_specs, out_specs=out_specs, check_vma=False)
```

```python
import jax
import jax.numpy as jnp
from jax import lax
from jax.experimental import pallas as pl
from jax.experimental.pallas import tpu as pltpu
from jax.sharding import Mesh, PartitionSpec as P

LEN = 128
EPSILON = 1e-06
Z_LO = 8
Z = ("rep", "zl")
SWAP = [(0, 1), (1, 0)]

VMEM = pl.BlockSpec(memory_space=pltpu.VMEM)
SMEM = pl.BlockSpec(memory_space=pltpu.SMEM)


def shift(value, axis, size, distance):
    return lax.ppermute(value, axis, [((k + distance) % size, k) for k in range(size)])


def exchange(blocks, axis):
    return lax.all_to_all(blocks, axis, 0, 0, tiled=True)


def rms_scale(values, gain):
    return values * lax.rsqrt(jnp.mean(values * values, axis=-1, keepdims=True) + EPSILON) * gain


def dot_t(acts, weight_t):
    return lax.dot_general(acts, weight_t, (((1,), (1,)), ((), ())), preferred_element_type=jnp.float32)


def dot(acts, weight):
    return jnp.dot(acts, weight, preferred_element_type=jnp.float32)


def call(kernel, outs, pos, args, mib, scratch=(), placed=True):
    if placed:
        args = [pltpu.with_memory_space_constraint(a, pltpu.VMEM) for a in args]
    specs = [VMEM] * len(args)
    if pos is not None:
        args, specs = [pos, *args], [SMEM, *specs]
    return pl.pallas_call(
        kernel,
        out_shape=outs,
        in_specs=specs,
        out_specs=(VMEM,) * len(outs),
        scratch_shapes=scratch,
        compiler_params=pltpu.CompilerParams(vmem_limit_bytes=mib * 1024 * 1024),
    )(*args)


def mixer_kernel(pos, normed, taps, gathered, mine, other, weights, gated):
    core = pos[1]
    n_y, n_z, rows, _ = gathered.shape
    width = taps.shape[1]
    for z in range(n_z):
        for y in range(n_y):
            first = (z * n_y + y) * rows
            weights[first : first + rows, :] = gathered[y, z]
    products = dot(normed[...], weights[:, : 3 * width])
    p = products[:, width : 2 * width] * products[:, 2 * width : 3 * width]
    place = lax.broadcasted_iota(jnp.int32, p.shape, 0) % LEN
    before = jnp.where(place >= 1, pltpu.roll(p, 1, 0), 0.0)
    before_two = jnp.where(place >= 2, pltpu.roll(p, 2, 0), 0.0)
    convolved = taps[0:1, :] * before_two + taps[1:2, :] * before + taps[2:3, :] * p
    gated[...] = (products[:, :width] * convolved).astype(jnp.bfloat16)
    out_t = weights[:, 3 * width :]
    n_x = mine.shape[0]
    step = mine.shape[1]
    for half, out in ((core, mine), (1 - core, other)):
        for x in range(n_x):
            first = pl.multiple_of(x * 2 * step + half * step, step)
            out[x] = dot_t(gated[pl.ds(first, step), :], out_t).astype(jnp.bfloat16)


def tick_kernel(pos, out):
    for k in range(pos.shape[0]):
        out[k] = pos[k]


def tick(pos):
    return pl.pallas_call(
        tick_kernel,
        out_shape=jax.ShapeDtypeStruct(pos.shape, pos.dtype),
        in_specs=[SMEM],
        out_specs=SMEM,
        compiler_params=pltpu.CompilerParams(vmem_limit_bytes=1024 * 1024),
    )(pos)


def ordered_kernel(places, pos, *refs):
    out = refs[-1]
    for d, block in zip(places, refs[:-1]):
        y = lax.rem(pos[2] + (d + len(places)), len(places))
        out[pl.ds(pl.multiple_of(y * block.shape[0], block.shape[0]), block.shape[0]), :] = block[...]


def copy_kernel(block, out):
    out[0] = block[...]


def bundle_kernel(*refs):
    out = refs[-1]
    out[...] = jnp.zeros(out.shape, out.dtype)
    step = out.shape[2] // (len(refs) - 1)
    for k, array in enumerate(refs[:-1]):
        out[0, :, k * step : k * step + array.shape[1]] = array[...]


def for_exchange(kernel, args, count, shape, dtype, space=pltpu.HBM, source=pltpu.HBM):
    args = [pltpu.with_memory_space_constraint(a, source) for a in args]
    zeros = (0,) * len(shape)
    return pl.pallas_call(
        kernel,
        grid=(count,),
        out_shape=space((count, *shape), dtype),
        in_specs=[VMEM] * len(args),
        out_specs=pl.BlockSpec((1, *shape), lambda k: (k, *zeros)),
        compiler_params=pltpu.CompilerParams(vmem_limit_bytes=8 * 1024 * 1024),
    )(*args)


def join_kernel(blocks, own, gain, stream, sent):
    total = own[...].astype(jnp.float32)
    for k in range(blocks.shape[0]):
        total += blocks[k].astype(jnp.float32)
    stream[...] = total
    normed = rms_scale(total, gain[...]).astype(jnp.bfloat16)
    for k in range(sent.shape[0]):
        sent[k] = normed


def last_kernel(blocks, stream, out):
    total = stream[...]
    for k in range(blocks.shape[0]):
        total += blocks[k].astype(jnp.float32)
    out[...] = total.astype(jnp.bfloat16)


def ffn_kernel(places, n_ff, pos, acts, acts_other, *refs):
    chunks, out, out_other = refs[: len(places)], refs[len(places)], refs[len(places) + 1]
    depth = acts.shape[1] // Z_LO
    step = chunks[0].shape[1] // 3
    both = None
    firsts = []
    for (d, row), chunk in zip(places, chunks):
        z = lax.rem(pos[0] + (d + Z_LO), Z_LO)
        first = pl.multiple_of(z * depth + row, chunk.shape[0])
        firsts.append(first)
        columns = pl.ds(first, chunk.shape[0])
        values = jnp.concatenate([acts[:, columns], acts_other[:, columns]], axis=0)
        part = dot(values, chunk[:, : 2 * step])
        both = part if both is None else both + part
    hidden = (jax.nn.silu(both[:, :n_ff]) * both[:, step : step + n_ff]).astype(jnp.bfloat16)
    half = acts.shape[0]
    for first, chunk in zip(firsts, chunks):
        part = dot_t(hidden, chunk[:, 2 * step : 2 * step + n_ff]).astype(jnp.bfloat16)
        columns = pl.ds(first, chunk.shape[0])
        out[:, columns] = part[:half]
        out_other[:, columns] = part[half:]


def local(
    tokens,
    mix_gain,
    w_gate_b,
    w_gate_c,
    w_conv_in,
    conv_taps,
    w_mix_out,
    ffn_gain,
    w_ffn_gate,
    w_ffn_up,
    w_ffn_down,
):
    nx, ny = lax.axis_size("x"), lax.axis_size("y")
    nz = lax.axis_size("rep") * lax.axis_size("zl")
    zl, core = lax.axis_index("zl"), lax.axis_index("core")
    pos = jnp.stack([zl, core, lax.axis_index("y")]).astype(jnp.int32)
    count, feats = tokens.shape
    half_rows = count // 2
    own_rows = half_rows // nx

    mixer = jnp.concatenate([w_gate_b, w_gate_c, w_conv_in, w_mix_out.T], axis=1)
    mixer_shape = mixer.shape
    sent = jnp.broadcast_to(mixer[None], (Z_LO, *mixer_shape))
    along_z = exchange(sent, "zl")
    sent = for_exchange(copy_kernel, (along_z,), ny, along_z.shape, along_z.dtype, source=pltpu.VMEM)
    normed = rms_scale(tokens.astype(jnp.float32), mix_gain).astype(jnp.bfloat16)
    own = lax.dynamic_slice_in_dim(tokens, (lax.axis_index("x") * 2 + core) * own_rows, own_rows, 0)
    gathered = exchange(sent.reshape(-1, *mixer_shape), "y").reshape(ny, Z_LO, *mixer_shape)

    n_ff = w_ffn_gate.shape[1]
    width = 3 * (-(-n_ff // 128) * 128)
    ffn_shape = (w_ffn_gate.shape[0], width)
    parts = (w_ffn_gate, w_ffn_up, w_ffn_down.T)
    ffn = for_exchange(bundle_kernel, parts, 1, ffn_shape, w_ffn_gate.dtype, jax.ShapeDtypeStruct)[0]
    y_places = [0, 2, 1, -1]
    blocks = [shift(ffn, "y", ny, d) if d else ffn for d in y_places]

    def ordered_body(*refs):
        ordered_kernel(y_places, *refs)

    (ffn_y,) = call(ordered_body, (jax.ShapeDtypeStruct((ny * ffn_shape[0], width), ffn.dtype),), pos, blocks, 4, placed=False)
    chunks, ffn_places = [ffn_y], [(0, 0)]
    up = down = ffn_y
    for k in (1, 2, 3):
        up, down = shift(up, Z, nz, 1), shift(down, Z, nz, -1)
        chunks += [up, down]
        ffn_places += [(k, 0), (-k, 0)]
    cut = ffn_y.shape[0] // 2
    chunks += [shift(up[:cut], Z, nz, 1), shift(down[cut:], Z, nz, -1)]
    ffn_places += [(4, 0), (4, cut)]

    bf, f32 = jnp.bfloat16, jnp.float32
    halves = (nx, own_rows, feats)

    pos = tick(pos)
    scratch = [pltpu.VMEM((feats, mixer_shape[1]), bf), pltpu.VMEM((count, w_gate_b.shape[1]), bf)]
    mine, other = call(mixer_kernel, (pltpu.VMEM(halves, bf),) * 2, pos, (normed, conv_taps, gathered), 16, scratch)

    def over_tp(mine, other):
        got = lax.ppermute(other, "core", SWAP)
        pair = (mine.astype(f32) + got.astype(f32)).astype(bf)
        return exchange(pair, "x")

    pos = tick(pos)
    blocks = over_tp(mine, other)
    stream, sent = call(
        join_kernel,
        (jax.ShapeDtypeStruct((own_rows, feats), f32), pltpu.HBM(halves, bf)),
        None,
        (blocks, own, ffn_gain.reshape(1, -1)),
        8,
    )
    pos = tick(pos)
    acts = exchange(sent, "x").reshape(half_rows, feats)
    acts_other = lax.ppermute(acts, "core", SWAP)

    def ffn_body(*refs):
        ffn_kernel(ffn_places, n_ff, *refs)

    pair = call(ffn_body, (pltpu.VMEM((half_rows, feats), bf),) * 2, pos, (acts, acts_other, *chunks), 24)
    blocks = over_tp(*(part.reshape(halves) for part in pair))
    return call(last_kernel, (jax.ShapeDtypeStruct((own_rows, feats), bf),), None, (blocks, stream), 8)[0]


def solution(mesh):
    fine = Mesh(
        mesh.devices.reshape(mesh.shape["rep"], Z_LO, mesh.shape["fs"] // Z_LO, mesh.shape["tp"] // 2, 2),
        ("rep", "zl", "y", "x", "core"),
    )
    fs, tp = ("zl", "y"), ("x", "core")
    in_specs = (
        P(("rep", *fs), None),
        P(),
        P(fs, tp),
        P(fs, tp),
        P(fs, tp),
        P(None, tp),
        P(tp, fs),
        P(),
        P(fs, tp),
        P(fs, tp),
        P(tp, fs),
    )
    out_specs = P(("rep", *fs, *tp), None)
    return jax.shard_map(local, mesh=fine, in_specs=in_specs, out_specs=out_specs, check_vma=False)
```

```python
import jax
import jax.numpy as jnp
from jax import lax
from jax.experimental import pallas as pl
from jax.experimental.pallas import tpu as pltpu
from jax.sharding import Mesh, PartitionSpec as P

LEN = 128
EPSILON = 1e-06
Z_LO = 8
Z = ("rep", "zl")
SWAP = [(0, 1), (1, 0)]

VMEM = pl.BlockSpec(memory_space=pltpu.VMEM)
ANY = pl.BlockSpec(memory_space=pl.ANY)
SMEM = pl.BlockSpec(memory_space=pltpu.SMEM)


def shift(value, axis, size, distance):
    return lax.ppermute(value, axis, [((k + distance) % size, k) for k in range(size)])


def exchange(blocks, axis):
    return lax.all_to_all(blocks, axis, 0, 0, tiled=True)


def rms_scale(values, gain):
    return values * lax.rsqrt(jnp.mean(values * values, axis=-1, keepdims=True) + EPSILON) * gain


def dot_t(acts, weight_t):
    return lax.dot_general(acts, weight_t, (((1,), (1,)), ((), ())), preferred_element_type=jnp.float32)


def dot(acts, weight):
    return jnp.dot(acts, weight, preferred_element_type=jnp.float32)


def call(kernel, outs, pos, args, mib, scratch=(), far=()):
    args = [pltpu.with_memory_space_constraint(a, pltpu.VMEM) for a in args]
    specs = [VMEM] * len(args) + [ANY] * len(far)
    args += [pltpu.with_memory_space_constraint(a, pltpu.HBM) for a in far]
    if pos is not None:
        args, specs = [pos, *args], [SMEM, *specs]
    return pl.pallas_call(
        kernel,
        out_shape=outs,
        in_specs=specs,
        out_specs=(VMEM,) * len(outs),
        scratch_shapes=scratch,
        compiler_params=pltpu.CompilerParams(vmem_limit_bytes=mib * 1024 * 1024),
    )(*args)


def mixer_kernel(pos, normed, taps, gathered, mine, other, weights, gated, sems):
    core = pos[1]
    n_y, n_z, rows, _ = gathered.shape
    fetches = [
        pltpu.make_async_copy(gathered.at[y, z], weights.at[pl.ds((z * n_y + y) * rows, rows)], sems.at[y, z])
        for y in range(n_y)
        for z in range(n_z)
    ]
    for fetch in fetches:
        fetch.start()
    for fetch in fetches:
        fetch.wait()
    width = taps.shape[1]
    products = dot(normed[...], weights[:, : 3 * width])
    p = products[:, width : 2 * width] * products[:, 2 * width : 3 * width]
    place = lax.broadcasted_iota(jnp.int32, p.shape, 0) % LEN
    before = jnp.where(place >= 1, pltpu.roll(p, 1, 0), 0.0)
    before_two = jnp.where(place >= 2, pltpu.roll(p, 2, 0), 0.0)
    convolved = taps[0:1, :] * before_two + taps[1:2, :] * before + taps[2:3, :] * p
    gated[...] = (products[:, :width] * convolved).astype(jnp.bfloat16)
    out_t = weights[:, 3 * width :]
    n_x = mine.shape[0]
    step = mine.shape[1]
    for half, out in ((core, mine), (1 - core, other)):
        for x in range(n_x):
            first = pl.multiple_of(x * 2 * step + half * step, step)
            out[x] = dot_t(gated[pl.ds(first, step), :], out_t).astype(jnp.bfloat16)


def tick_kernel(pos, out):
    for k in range(pos.shape[0]):
        out[k] = pos[k]


def tick(pos):
    return pl.pallas_call(
        tick_kernel,
        out_shape=jax.ShapeDtypeStruct(pos.shape, pos.dtype),
        in_specs=[SMEM],
        out_specs=SMEM,
        compiler_params=pltpu.CompilerParams(vmem_limit_bytes=1024 * 1024),
    )(pos)


def ordered_kernel(places, pos, *refs):
    out = refs[-1]
    for d, block in zip(places, refs[:-1]):
        y = lax.rem(pos[2] + (d + len(places)), len(places))
        out[pl.ds(pl.multiple_of(y * block.shape[0], block.shape[0]), block.shape[0]), :] = block[...]


def copy_kernel(block, out):
    out[0] = block[...]


def bundle_kernel(*refs):
    out = refs[-1]
    out[...] = jnp.zeros(out.shape, out.dtype)
    step = out.shape[2] // (len(refs) - 1)
    for k, array in enumerate(refs[:-1]):
        out[0, :, k * step : k * step + array.shape[1]] = array[...]


def for_exchange(kernel, args, count, shape, dtype, space=pltpu.HBM, source=pltpu.HBM):
    args = [pltpu.with_memory_space_constraint(a, source) for a in args]
    zeros = (0,) * len(shape)
    return pl.pallas_call(
        kernel,
        grid=(count,),
        out_shape=space((count, *shape), dtype),
        in_specs=[VMEM] * len(args),
        out_specs=pl.BlockSpec((1, *shape), lambda k: (k, *zeros)),
        compiler_params=pltpu.CompilerParams(vmem_limit_bytes=8 * 1024 * 1024),
    )(*args)


def join_kernel(blocks, own, gain, stream, sent):
    total = own[...].astype(jnp.float32)
    for k in range(blocks.shape[0]):
        total += blocks[k].astype(jnp.float32)
    stream[...] = total
    normed = rms_scale(total, gain[...]).astype(jnp.bfloat16)
    for k in range(sent.shape[0]):
        sent[k] = normed


def last_kernel(blocks, stream, out):
    total = stream[...]
    for k in range(blocks.shape[0]):
        total += blocks[k].astype(jnp.float32)
    out[...] = total.astype(jnp.bfloat16)


def ffn_kernel(places, n_ff, pos, acts, acts_other, *refs):
    count = len(places)
    chunks, (out, out_other, *rest) = refs[:count], refs[count:]
    weights, sems = rest[:count], rest[count]
    depth = acts.shape[1] // Z_LO
    step = chunks[0].shape[1] // 3
    fetches = [pltpu.make_async_copy(chunks[k], weights[k], sems.at[k]) for k in range(count)]
    for fetch in fetches:
        fetch.start()
    both = None
    firsts = []
    for (d, row), chunk, fetch in zip(places, weights, fetches):
        z = lax.rem(pos[0] + (d + Z_LO), Z_LO)
        first = pl.multiple_of(z * depth + row, chunk.shape[0])
        firsts.append(first)
        columns = pl.ds(first, chunk.shape[0])
        values = jnp.concatenate([acts[:, columns], acts_other[:, columns]], axis=0)
        fetch.wait()
        part = dot(values, chunk[:, : 2 * step])
        both = part if both is None else both + part
    hidden = (jax.nn.silu(both[:, :n_ff]) * both[:, step : step + n_ff]).astype(jnp.bfloat16)
    half = acts.shape[0]
    for first, chunk in zip(firsts, weights):
        part = dot_t(hidden, chunk[:, 2 * step : 2 * step + n_ff]).astype(jnp.bfloat16)
        columns = pl.ds(first, chunk.shape[0])
        out[:, columns] = part[:half]
        out_other[:, columns] = part[half:]


def local(
    tokens,
    mix_gain,
    w_gate_b,
    w_gate_c,
    w_conv_in,
    conv_taps,
    w_mix_out,
    ffn_gain,
    w_ffn_gate,
    w_ffn_up,
    w_ffn_down,
):
    nx, ny = lax.axis_size("x"), lax.axis_size("y")
    nz = lax.axis_size("rep") * lax.axis_size("zl")
    zl, core = lax.axis_index("zl"), lax.axis_index("core")
    pos = jnp.stack([zl, core, lax.axis_index("y")]).astype(jnp.int32)
    count, feats = tokens.shape
    half_rows = count // 2
    own_rows = half_rows // nx

    mixer = jnp.concatenate([w_gate_b, w_gate_c, w_conv_in, w_mix_out.T], axis=1)
    mixer_shape = mixer.shape
    sent = jnp.broadcast_to(mixer[None], (Z_LO, *mixer_shape))
    along_z = exchange(sent, "zl")
    sent = for_exchange(copy_kernel, (along_z,), ny, along_z.shape, along_z.dtype, source=pltpu.VMEM)
    normed = rms_scale(tokens.astype(jnp.float32), mix_gain).astype(jnp.bfloat16)
    own = lax.dynamic_slice_in_dim(tokens, (lax.axis_index("x") * 2 + core) * own_rows, own_rows, 0)
    gathered = exchange(sent.reshape(-1, *mixer_shape), "y").reshape(ny, Z_LO, *mixer_shape)

    n_ff = w_ffn_gate.shape[1]
    width = 3 * (-(-n_ff // 128) * 128)
    ffn_shape = (w_ffn_gate.shape[0], width)
    parts = (w_ffn_gate, w_ffn_up, w_ffn_down.T)
    ffn = for_exchange(bundle_kernel, parts, 1, ffn_shape, w_ffn_gate.dtype, jax.ShapeDtypeStruct)[0]
    y_places = [0, 2, 1, -1]
    blocks = [shift(ffn, "y", ny, d) if d else ffn for d in y_places]

    def ordered_body(*refs):
        ordered_kernel(y_places, *refs)

    (ffn_y,) = call(ordered_body, (jax.ShapeDtypeStruct((ny * ffn_shape[0], width), ffn.dtype),), pos, blocks, 4)
    chunks, ffn_places = [ffn_y], [(0, 0)]
    up = down = ffn_y
    for k in (1, 2, 3):
        up, down = shift(up, Z, nz, 1), shift(down, Z, nz, -1)
        chunks += [up, down]
        ffn_places += [(k, 0), (-k, 0)]
    cut = ffn_y.shape[0] // 2
    chunks += [shift(up[:cut], Z, nz, 1), shift(down[cut:], Z, nz, -1)]
    ffn_places += [(4, 0), (4, cut)]

    bf, f32 = jnp.bfloat16, jnp.float32
    halves = (nx, own_rows, feats)

    pos = tick(pos)
    scratch = [
        pltpu.VMEM((feats, mixer_shape[1]), bf),
        pltpu.VMEM((count, w_gate_b.shape[1]), bf),
        pltpu.SemaphoreType.DMA((ny, Z_LO)),
    ]
    mine, other = call(
        mixer_kernel, (pltpu.VMEM(halves, bf),) * 2, pos, (normed, conv_taps), 16, scratch, (gathered,)
    )

    def over_tp(mine, other):
        got = lax.ppermute(other, "core", SWAP)
        pair = (mine.astype(f32) + got.astype(f32)).astype(bf)
        return exchange(pair, "x")

    pos = tick(pos)
    blocks = over_tp(mine, other)
    stream, sent = call(
        join_kernel,
        (jax.ShapeDtypeStruct((own_rows, feats), f32), pltpu.HBM(halves, bf)),
        None,
        (blocks, own, ffn_gain.reshape(1, -1)),
        8,
    )
    pos = tick(pos)
    acts = exchange(sent, "x").reshape(half_rows, feats)
    acts_other = lax.ppermute(acts, "core", SWAP)

    def ffn_body(*refs):
        ffn_kernel(ffn_places, n_ff, *refs)

    room = [pltpu.VMEM(chunk.shape, bf) for chunk in chunks] + [pltpu.SemaphoreType.DMA((len(chunks),))]
    pair = call(ffn_body, (pltpu.VMEM((half_rows, feats), bf),) * 2, pos, (acts, acts_other), 24, room, chunks)
    blocks = over_tp(*(part.reshape(halves) for part in pair))
    return call(last_kernel, (jax.ShapeDtypeStruct((own_rows, feats), bf),), None, (blocks, stream), 8)[0]


def solution(mesh):
    fine = Mesh(
        mesh.devices.reshape(mesh.shape["rep"], Z_LO, mesh.shape["fs"] // Z_LO, mesh.shape["tp"] // 2, 2),
        ("rep", "zl", "y", "x", "core"),
    )
    fs, tp = ("zl", "y"), ("x", "core")
    in_specs = (
        P(("rep", *fs), None),
        P(),
        P(fs, tp),
        P(fs, tp),
        P(fs, tp),
        P(None, tp),
        P(tp, fs),
        P(),
        P(fs, tp),
        P(fs, tp),
        P(tp, fs),
    )
    out_specs = P(("rep", *fs, *tp), None)
    return jax.shard_map(local, mesh=fine, in_specs=in_specs, out_specs=out_specs, check_vma=False)
```

```python
import jax
import jax.numpy as jnp
from jax import lax
from jax.experimental import pallas as pl
from jax.experimental.pallas import tpu as pltpu
from jax.sharding import Mesh, PartitionSpec as P

LEN = 128
EPSILON = 1e-06
Z_LO = 8
Z = ("rep", "zl")
SWAP = [(0, 1), (1, 0)]

VMEM = pl.BlockSpec(memory_space=pltpu.VMEM)
ANY = pl.BlockSpec(memory_space=pl.ANY)
SMEM = pl.BlockSpec(memory_space=pltpu.SMEM)


def shift(value, axis, size, distance):
    return lax.ppermute(value, axis, [((k + distance) % size, k) for k in range(size)])


def exchange(blocks, axis):
    return lax.all_to_all(blocks, axis, 0, 0, tiled=True)


def rms_scale(values, gain):
    return values * lax.rsqrt(jnp.mean(values * values, axis=-1, keepdims=True) + EPSILON) * gain


def dot_t(acts, weight_t):
    return lax.dot_general(acts, weight_t, (((1,), (1,)), ((), ())), preferred_element_type=jnp.float32)


def dot(acts, weight):
    return jnp.dot(acts, weight, preferred_element_type=jnp.float32)


def call(kernel, outs, pos, args, mib, scratch=(), far=()):
    args = [pltpu.with_memory_space_constraint(a, pltpu.VMEM) for a in args]
    specs = [VMEM] * len(args) + [ANY] * len(far)
    args += [pltpu.with_memory_space_constraint(a, pltpu.HBM) for a in far]
    if pos is not None:
        args, specs = [pos, *args], [SMEM, *specs]
    return pl.pallas_call(
        kernel,
        out_shape=outs,
        in_specs=specs,
        out_specs=(VMEM,) * len(outs),
        scratch_shapes=scratch,
        compiler_params=pltpu.CompilerParams(vmem_limit_bytes=mib * 1024 * 1024),
    )(*args)


def mixer_kernel(pos, normed, taps, gathered, mine, other, weights, gated):
    core = pos[1]
    n_y, n_z, rows, _ = gathered.shape
    width = taps.shape[1]
    for z in range(n_z):
        for y in range(n_y):
            first = (z * n_y + y) * rows
            weights[first : first + rows, :] = gathered[y, z]
    products = dot(normed[...], weights[:, : 3 * width])
    p = products[:, width : 2 * width] * products[:, 2 * width : 3 * width]
    place = lax.broadcasted_iota(jnp.int32, p.shape, 0) % LEN
    before = jnp.where(place >= 1, pltpu.roll(p, 1, 0), 0.0)
    before_two = jnp.where(place >= 2, pltpu.roll(p, 2, 0), 0.0)
    convolved = taps[0:1, :] * before_two + taps[1:2, :] * before + taps[2:3, :] * p
    gated[...] = (products[:, :width] * convolved).astype(jnp.bfloat16)
    out_t = weights[:, 3 * width :]
    n_x = mine.shape[0]
    step = mine.shape[1]
    for half, out in ((core, mine), (1 - core, other)):
        for x in range(n_x):
            first = pl.multiple_of(x * 2 * step + half * step, step)
            out[x] = dot_t(gated[pl.ds(first, step), :], out_t).astype(jnp.bfloat16)


def tick_kernel(pos, out):
    for k in range(pos.shape[0]):
        out[k] = pos[k]


def tick(pos):
    return pl.pallas_call(
        tick_kernel,
        out_shape=jax.ShapeDtypeStruct(pos.shape, pos.dtype),
        in_specs=[SMEM],
        out_specs=SMEM,
        compiler_params=pltpu.CompilerParams(vmem_limit_bytes=1024 * 1024),
    )(pos)


def ordered_kernel(places, pos, *refs):
    out = refs[-1]
    for d, block in zip(places, refs[:-1]):
        y = lax.rem(pos[2] + (d + len(places)), len(places))
        out[pl.ds(pl.multiple_of(y * block.shape[0], block.shape[0]), block.shape[0]), :] = block[...]


def copies_kernel(block, out, sems):
    fetches = [pltpu.make_async_copy(block, out.at[k], sems.at[k]) for k in range(out.shape[0])]
    for fetch in fetches:
        fetch.start()
    for fetch in fetches:
        fetch.wait()


def bundle_kernel(*refs):
    out = refs[-1]
    out[...] = jnp.zeros(out.shape, out.dtype)
    step = out.shape[2] // (len(refs) - 1)
    for k, array in enumerate(refs[:-1]):
        out[0, :, k * step : k * step + array.shape[1]] = array[...]


def for_exchange(kernel, args, count, shape, dtype, space=pltpu.HBM, source=pltpu.HBM):
    args = [pltpu.with_memory_space_constraint(a, source) for a in args]
    zeros = (0,) * len(shape)
    return pl.pallas_call(
        kernel,
        grid=(count,),
        out_shape=space((count, *shape), dtype),
        in_specs=[VMEM] * len(args),
        out_specs=pl.BlockSpec((1, *shape), lambda k: (k, *zeros)),
        compiler_params=pltpu.CompilerParams(vmem_limit_bytes=8 * 1024 * 1024),
    )(*args)


def join_kernel(blocks, own, gain, stream, sent):
    total = own[...].astype(jnp.float32)
    for k in range(blocks.shape[0]):
        total += blocks[k].astype(jnp.float32)
    stream[...] = total
    normed = rms_scale(total, gain[...]).astype(jnp.bfloat16)
    for k in range(sent.shape[0]):
        sent[k] = normed


def last_kernel(blocks, stream, out):
    total = stream[...]
    for k in range(blocks.shape[0]):
        total += blocks[k].astype(jnp.float32)
    out[...] = total.astype(jnp.bfloat16)


def ffn_kernel(places, n_ff, pos, acts, acts_other, *refs):
    count = len(places)
    chunks, (out, out_other, weights, values, sems) = refs[:count], refs[count:]
    half = acts.shape[0]
    depth = acts.shape[1] // Z_LO
    step = weights.shape[1] // 3
    fetches, spans = [], []
    at = 0
    for k, ((d, row), chunk) in enumerate(zip(places, chunks)):
        rows = chunk.shape[0]
        fetches.append(pltpu.make_async_copy(chunk, weights.at[at : at + rows], sems.at[k]))
        fetches[-1].start()
        z = lax.rem(pos[0] + (d + Z_LO), Z_LO)
        spans.append((at, rows, pl.ds(pl.multiple_of(z * depth + row, rows), rows)))
        at += rows
    for first, rows, columns in spans:
        values[:half, first : first + rows] = acts[:, columns]
        values[half:, first : first + rows] = acts_other[:, columns]
    middle = at // 2
    for fetch, (first, _, _) in zip(fetches, spans):
        if first < middle:
            fetch.wait()
    both = dot(values[:, :middle], weights[:middle, : 2 * step])
    for fetch, (first, _, _) in zip(fetches, spans):
        if first >= middle:
            fetch.wait()
    both += dot(values[:, middle:], weights[middle:, : 2 * step])
    hidden = (jax.nn.silu(both[:, :n_ff]) * both[:, step : step + n_ff]).astype(jnp.bfloat16)
    for first, rows, columns in spans:
        part = dot_t(hidden, weights[first : first + rows, 2 * step : 2 * step + n_ff]).astype(jnp.bfloat16)
        out[:, columns] = part[:half]
        out_other[:, columns] = part[half:]


def local(
    tokens,
    mix_gain,
    w_gate_b,
    w_gate_c,
    w_conv_in,
    conv_taps,
    w_mix_out,
    ffn_gain,
    w_ffn_gate,
    w_ffn_up,
    w_ffn_down,
):
    nx, ny = lax.axis_size("x"), lax.axis_size("y")
    nz = lax.axis_size("rep") * lax.axis_size("zl")
    zl, core = lax.axis_index("zl"), lax.axis_index("core")
    pos = jnp.stack([zl, core, lax.axis_index("y")]).astype(jnp.int32)
    count, feats = tokens.shape
    half_rows = count // 2
    own_rows = half_rows // nx

    mixer = jnp.concatenate([w_gate_b, w_gate_c, w_conv_in, w_mix_out.T], axis=1)
    mixer_shape = mixer.shape
    sent = jnp.broadcast_to(mixer[None], (Z_LO, *mixer_shape))
    along_z = exchange(sent, "zl")
    sent = pl.pallas_call(
        copies_kernel,
        out_shape=pltpu.HBM((ny, *along_z.shape), along_z.dtype),
        in_specs=[VMEM],
        out_specs=ANY,
        scratch_shapes=[pltpu.SemaphoreType.DMA((ny,))],
        compiler_params=pltpu.CompilerParams(vmem_limit_bytes=4 * 1024 * 1024),
    )(pltpu.with_memory_space_constraint(along_z, pltpu.VMEM))
    normed = rms_scale(tokens.astype(jnp.float32), mix_gain).astype(jnp.bfloat16)
    own = lax.dynamic_slice_in_dim(tokens, (lax.axis_index("x") * 2 + core) * own_rows, own_rows, 0)
    gathered = exchange(sent.reshape(-1, *mixer_shape), "y").reshape(ny, Z_LO, *mixer_shape)

    n_ff = w_ffn_gate.shape[1]
    width = 3 * (-(-n_ff // 128) * 128)
    ffn_shape = (w_ffn_gate.shape[0], width)
    parts = (w_ffn_gate, w_ffn_up, w_ffn_down.T)
    ffn = for_exchange(bundle_kernel, parts, 1, ffn_shape, w_ffn_gate.dtype, jax.ShapeDtypeStruct)[0]
    y_places = [0, 2, 1, -1]
    blocks = [shift(ffn, "y", ny, d) if d else ffn for d in y_places]

    def ordered_body(*refs):
        ordered_kernel(y_places, *refs)

    (ffn_y,) = call(ordered_body, (jax.ShapeDtypeStruct((ny * ffn_shape[0], width), ffn.dtype),), pos, blocks, 4)
    chunks, ffn_places = [ffn_y], [(0, 0)]
    up = down = ffn_y
    for k in (1, 2, 3):
        up, down = shift(up, Z, nz, 1), shift(down, Z, nz, -1)
        chunks += [up, down]
        ffn_places += [(k, 0), (-k, 0)]
    cut = ffn_y.shape[0] // 2
    chunks += [shift(up[:cut], Z, nz, 1), shift(down[cut:], Z, nz, -1)]
    ffn_places += [(4, 0), (4, cut)]

    bf, f32 = jnp.bfloat16, jnp.float32
    halves = (nx, own_rows, feats)

    pos = tick(pos)
    scratch = [
        pltpu.VMEM((feats, mixer_shape[1]), bf),
        pltpu.VMEM((count, w_gate_b.shape[1]), bf),
    ]
    mine, other = call(
        mixer_kernel, (pltpu.VMEM(halves, bf),) * 2, pos, (normed, conv_taps, gathered), 16, scratch
    )

    def over_tp(mine, other):
        got = lax.ppermute(other, "core", SWAP)
        pair = (mine.astype(f32) + got.astype(f32)).astype(bf)
        return exchange(pair, "x")

    pos = tick(pos)
    blocks = over_tp(mine, other)
    stream, sent = call(
        join_kernel,
        (jax.ShapeDtypeStruct((own_rows, feats), f32), pltpu.HBM(halves, bf)),
        None,
        (blocks, own, ffn_gain.reshape(1, -1)),
        8,
    )
    pos = tick(pos)
    acts = exchange(sent, "x").reshape(half_rows, feats)
    acts_other = lax.ppermute(acts, "core", SWAP)

    def ffn_body(*refs):
        ffn_kernel(ffn_places, n_ff, *refs)

    room = [
        pltpu.VMEM((feats, width), bf),
        pltpu.VMEM((count, feats), bf),
        pltpu.SemaphoreType.DMA((len(chunks),)),
    ]
    pair = call(ffn_body, (pltpu.VMEM((half_rows, feats), bf),) * 2, pos, (acts, acts_other), 24, room, chunks)
    blocks = over_tp(*(part.reshape(halves) for part in pair))
    return call(last_kernel, (jax.ShapeDtypeStruct((own_rows, feats), bf),), None, (blocks, stream), 8)[0]


def solution(mesh):
    fine = Mesh(
        mesh.devices.reshape(mesh.shape["rep"], Z_LO, mesh.shape["fs"] // Z_LO, mesh.shape["tp"] // 2, 2),
        ("rep", "zl", "y", "x", "core"),
    )
    fs, tp = ("zl", "y"), ("x", "core")
    in_specs = (
        P(("rep", *fs), None),
        P(),
        P(fs, tp),
        P(fs, tp),
        P(fs, tp),
        P(None, tp),
        P(tp, fs),
        P(),
        P(fs, tp),
        P(fs, tp),
        P(tp, fs),
    )
    out_specs = P(("rep", *fs, *tp), None)
    return jax.shard_map(local, mesh=fine, in_specs=in_specs, out_specs=out_specs, check_vma=False)
```

```python
import jax
import jax.numpy as jnp
from jax import lax
from jax.experimental import pallas as pl
from jax.experimental.pallas import tpu as pltpu
from jax.sharding import Mesh, PartitionSpec as P

LEN = 128
EPSILON = 1e-06
Z_LO = 8
Z = ("rep", "zl")
SWAP = [(0, 1), (1, 0)]

VMEM = pl.BlockSpec(memory_space=pltpu.VMEM)
ANY = pl.BlockSpec(memory_space=pl.ANY)
SMEM = pl.BlockSpec(memory_space=pltpu.SMEM)


def shift(value, axis, size, distance):
    return lax.ppermute(value, axis, [((k + distance) % size, k) for k in range(size)])


def exchange(blocks, axis):
    return lax.all_to_all(blocks, axis, 0, 0, tiled=True)


def rms_scale(values, gain):
    return values * lax.rsqrt(jnp.mean(values * values, axis=-1, keepdims=True) + EPSILON) * gain


def dot_t(acts, weight_t):
    return lax.dot_general(acts, weight_t, (((1,), (1,)), ((), ())), preferred_element_type=jnp.float32)


def dot(acts, weight):
    return jnp.dot(acts, weight, preferred_element_type=jnp.float32)


def call(kernel, outs, pos, args, mib, scratch=(), far=()):
    args = [pltpu.with_memory_space_constraint(a, pltpu.VMEM) for a in args]
    specs = [VMEM] * len(args) + [ANY] * len(far)
    args += [pltpu.with_memory_space_constraint(a, pltpu.HBM) for a in far]
    if pos is not None:
        args, specs = [pos, *args], [SMEM, *specs]
    return pl.pallas_call(
        kernel,
        out_shape=outs,
        in_specs=specs,
        out_specs=(VMEM,) * len(outs),
        scratch_shapes=scratch,
        compiler_params=pltpu.CompilerParams(vmem_limit_bytes=mib * 1024 * 1024),
    )(*args)


def mixer_kernel(pos, normed, taps, gathered, mine, other, weights, gated):
    core = pos[1]
    n_y, n_z, rows, _ = gathered.shape
    width = taps.shape[1]
    for z in range(n_z):
        for y in range(n_y):
            first = (z * n_y + y) * rows
            weights[first : first + rows, :] = gathered[y, z]
    products = dot(normed[...], weights[:, : 3 * width])
    p = products[:, width : 2 * width] * products[:, 2 * width : 3 * width]
    place = lax.broadcasted_iota(jnp.int32, p.shape, 0) % LEN
    before = jnp.where(place >= 1, pltpu.roll(p, 1, 0), 0.0)
    before_two = jnp.where(place >= 2, pltpu.roll(p, 2, 0), 0.0)
    convolved = taps[0:1, :] * before_two + taps[1:2, :] * before + taps[2:3, :] * p
    gated[...] = (products[:, :width] * convolved).astype(jnp.bfloat16)
    out_t = weights[:, 3 * width :]
    n_x = mine.shape[0]
    step = mine.shape[1]
    for half, out in ((core, mine), (1 - core, other)):
        for x in range(n_x):
            first = pl.multiple_of(x * 2 * step + half * step, step)
            out[x] = dot_t(gated[pl.ds(first, step), :], out_t).astype(jnp.bfloat16)


def tick_kernel(pos, out):
    for k in range(pos.shape[0]):
        out[k] = pos[k]


def tick(pos):
    return pl.pallas_call(
        tick_kernel,
        out_shape=jax.ShapeDtypeStruct(pos.shape, pos.dtype),
        in_specs=[SMEM],
        out_specs=SMEM,
        compiler_params=pltpu.CompilerParams(vmem_limit_bytes=1024 * 1024),
    )(pos)


def ordered_kernel(places, pos, *refs):
    out = refs[-1]
    for d, block in zip(places, refs[:-1]):
        y = lax.rem(pos[2] + (d + len(places)), len(places))
        out[pl.ds(pl.multiple_of(y * block.shape[0], block.shape[0]), block.shape[0]), :] = block[...]


def copies_kernel(block, out, sems):
    fetches = [pltpu.make_async_copy(block, out.at[k], sems.at[k]) for k in range(out.shape[0])]
    for fetch in fetches:
        fetch.start()
    for fetch in fetches:
        fetch.wait()


def bundle_kernel(*refs):
    out = refs[-1]
    out[...] = jnp.zeros(out.shape, out.dtype)
    step = out.shape[2] // (len(refs) - 1)
    for k, array in enumerate(refs[:-1]):
        out[0, :, k * step : k * step + array.shape[1]] = array[...]


def for_exchange(kernel, args, count, shape, dtype, space=pltpu.HBM, source=pltpu.HBM):
    args = [pltpu.with_memory_space_constraint(a, source) for a in args]
    zeros = (0,) * len(shape)
    return pl.pallas_call(
        kernel,
        grid=(count,),
        out_shape=space((count, *shape), dtype),
        in_specs=[VMEM] * len(args),
        out_specs=pl.BlockSpec((1, *shape), lambda k: (k, *zeros)),
        compiler_params=pltpu.CompilerParams(vmem_limit_bytes=8 * 1024 * 1024),
    )(*args)


def join_kernel(blocks, own, gain, stream, sent):
    total = own[...].astype(jnp.float32)
    for k in range(blocks.shape[0]):
        total += blocks[k].astype(jnp.float32)
    stream[...] = total
    normed = rms_scale(total, gain[...]).astype(jnp.bfloat16)
    for k in range(sent.shape[0]):
        sent[k] = normed


def last_kernel(blocks, stream, out):
    total = stream[...]
    for k in range(blocks.shape[0]):
        total += blocks[k].astype(jnp.float32)
    out[...] = total.astype(jnp.bfloat16)


def ffn_kernel(places, n_late, n_ff, pos, acts, acts_other, *refs):
    count = len(places)
    chunks, (out, out_other, weights, values, sems) = refs[:count], refs[count:]
    half = acts.shape[0]
    depth = acts.shape[1] // Z_LO
    step = weights.shape[1] // 3
    fetches, spans = [], []
    at = middle = 0
    for k, ((d, row), chunk) in enumerate(zip(places, chunks)):
        rows = chunk.shape[0]
        if k >= n_late:
            fetches.append(pltpu.make_async_copy(chunk, weights.at[at : at + rows], sems.at[k - n_late]))
            fetches[-1].start()
        z = lax.rem(pos[0] + (d + Z_LO), Z_LO)
        spans.append((at, rows, pl.ds(pl.multiple_of(z * depth + row, rows), rows)))
        at += rows
        if k < n_late:
            middle = at
    for k, (first, rows, columns) in enumerate(spans):
        if k < n_late:
            weights[first : first + rows, :] = chunks[k][...]
        values[:half, first : first + rows] = acts[:, columns]
        values[half:, first : first + rows] = acts_other[:, columns]
    both = dot(values[:, :middle], weights[:middle, : 2 * step])
    for fetch in fetches:
        fetch.wait()
    both += dot(values[:, middle:], weights[middle:, : 2 * step])
    hidden = (jax.nn.silu(both[:, :n_ff]) * both[:, step : step + n_ff]).astype(jnp.bfloat16)
    for first, rows, columns in spans:
        part = dot_t(hidden, weights[first : first + rows, 2 * step : 2 * step + n_ff]).astype(jnp.bfloat16)
        out[:, columns] = part[:half]
        out_other[:, columns] = part[half:]


def local(
    tokens,
    mix_gain,
    w_gate_b,
    w_gate_c,
    w_conv_in,
    conv_taps,
    w_mix_out,
    ffn_gain,
    w_ffn_gate,
    w_ffn_up,
    w_ffn_down,
):
    nx, ny = lax.axis_size("x"), lax.axis_size("y")
    nz = lax.axis_size("rep") * lax.axis_size("zl")
    zl, core = lax.axis_index("zl"), lax.axis_index("core")
    pos = jnp.stack([zl, core, lax.axis_index("y")]).astype(jnp.int32)
    count, feats = tokens.shape
    half_rows = count // 2
    own_rows = half_rows // nx

    mixer = jnp.concatenate([w_gate_b, w_gate_c, w_conv_in, w_mix_out.T], axis=1)
    mixer_shape = mixer.shape
    sent = jnp.broadcast_to(mixer[None], (Z_LO, *mixer_shape))
    along_z = exchange(sent, "zl")
    sent = pl.pallas_call(
        copies_kernel,
        out_shape=pltpu.HBM((ny, *along_z.shape), along_z.dtype),
        in_specs=[VMEM],
        out_specs=ANY,
        scratch_shapes=[pltpu.SemaphoreType.DMA((ny,))],
        compiler_params=pltpu.CompilerParams(vmem_limit_bytes=4 * 1024 * 1024),
    )(pltpu.with_memory_space_constraint(along_z, pltpu.VMEM))
    normed = rms_scale(tokens.astype(jnp.float32), mix_gain).astype(jnp.bfloat16)
    own = lax.dynamic_slice_in_dim(tokens, (lax.axis_index("x") * 2 + core) * own_rows, own_rows, 0)
    gathered = exchange(sent.reshape(-1, *mixer_shape), "y").reshape(ny, Z_LO, *mixer_shape)

    n_ff = w_ffn_gate.shape[1]
    width = 3 * (-(-n_ff // 128) * 128)
    ffn_shape = (w_ffn_gate.shape[0], width)
    parts = (w_ffn_gate, w_ffn_up, w_ffn_down.T)
    ffn = for_exchange(bundle_kernel, parts, 1, ffn_shape, w_ffn_gate.dtype, jax.ShapeDtypeStruct)[0]
    y_places = [0, 2, 1, -1]
    blocks = [shift(ffn, "y", ny, d) if d else ffn for d in y_places]

    def ordered_body(*refs):
        ordered_kernel(y_places, *refs)

    (ffn_y,) = call(ordered_body, (jax.ShapeDtypeStruct((ny * ffn_shape[0], width), ffn.dtype),), pos, blocks, 4)
    chunks, ffn_places = [ffn_y], [(0, 0)]
    up = down = ffn_y
    for k in (1, 2, 3):
        up, down = shift(up, Z, nz, 1), shift(down, Z, nz, -1)
        chunks += [up, down]
        ffn_places += [(k, 0), (-k, 0)]
    cut = ffn_y.shape[0] // 2
    chunks += [shift(up[:cut], Z, nz, 1), shift(down[cut:], Z, nz, -1)]
    ffn_places += [(4, 0), (4, cut)]

    bf, f32 = jnp.bfloat16, jnp.float32
    halves = (nx, own_rows, feats)

    pos = tick(pos)
    scratch = [
        pltpu.VMEM((feats, mixer_shape[1]), bf),
        pltpu.VMEM((count, w_gate_b.shape[1]), bf),
    ]
    mine, other = call(
        mixer_kernel, (pltpu.VMEM(halves, bf),) * 2, pos, (normed, conv_taps, gathered), 16, scratch
    )

    def over_tp(mine, other):
        got = lax.ppermute(other, "core", SWAP)
        pair = (mine.astype(f32) + got.astype(f32)).astype(bf)
        return exchange(pair, "x")

    pos = tick(pos)
    blocks = over_tp(mine, other)
    stream, sent = call(
        join_kernel,
        (jax.ShapeDtypeStruct((own_rows, feats), f32), pltpu.HBM(halves, bf)),
        None,
        (blocks, own, ffn_gain.reshape(1, -1)),
        8,
    )
    pos = tick(pos)
    acts = exchange(sent, "x").reshape(half_rows, feats)
    acts_other = lax.ppermute(acts, "core", SWAP)

    n_early = len(chunks) - 4
    order = [*range(n_early, len(chunks)), *range(n_early)]

    def ffn_body(*refs):
        ffn_kernel([ffn_places[k] for k in order], 4, n_ff, *refs)

    room = [
        pltpu.VMEM((feats, width), bf),
        pltpu.VMEM((count, feats), bf),
        pltpu.SemaphoreType.DMA((n_early,)),
    ]
    near, far = (acts, acts_other, *chunks[n_early:]), chunks[:n_early]
    pair = call(ffn_body, (pltpu.VMEM((half_rows, feats), bf),) * 2, pos, near, 14, room, far)
    blocks = over_tp(*(part.reshape(halves) for part in pair))
    return call(last_kernel, (jax.ShapeDtypeStruct((own_rows, feats), bf),), None, (blocks, stream), 8)[0]


def solution(mesh):
    fine = Mesh(
        mesh.devices.reshape(mesh.shape["rep"], Z_LO, mesh.shape["fs"] // Z_LO, mesh.shape["tp"] // 2, 2),
        ("rep", "zl", "y", "x", "core"),
    )
    fs, tp = ("zl", "y"), ("x", "core")
    in_specs = (
        P(("rep", *fs), None),
        P(),
        P(fs, tp),
        P(fs, tp),
        P(fs, tp),
        P(None, tp),
        P(tp, fs),
        P(),
        P(fs, tp),
        P(fs, tp),
        P(tp, fs),
    )
    out_specs = P(("rep", *fs, *tp), None)
    return jax.shard_map(local, mesh=fine, in_specs=in_specs, out_specs=out_specs, check_vma=False)
```
